32 devices in a mesh: grp: 2 (over y), sp: 4 (over z), fs: 2 (over x), tp: 2 (over core).
Axes of the slice: x: 2, y: 2, z: 4, core: 2. Of those that a mesh axis runs over, the one named last changes fastest.
Arguments:
- tokens: bfloat16 [8, 512, 2048], P(('grp', 'fs'), ('sp', 'tp')), parts along dimension 0, may hold values from -24 to 24
- norm_gain: float32 [2048], replicated, may hold values from 0.1 to 1.9
- w_query: bfloat16 [2048, 1024], P(('sp', 'fs'), 'tp'), may hold values from -0.125 to 0.125
- w_key: bfloat16 [2048, 1024], P(('sp', 'fs'), 'tp'), may hold values from -0.125 to 0.125
- w_value: bfloat16 [2048, 1024], P(('sp', 'fs'), 'tp'), may hold values from -0.125 to 0.125
- query_gain: float32 [1024], P('tp'), may hold values from 1 to 26
- key_gain: float32 [1024], P('tp'), may hold values from 0.1 to 1.9
- mix_lambda: float32 [8], P('tp'), may hold values from 0.3 to 0.8
- head_gain: float32 [128], replicated, may hold values from 0.1 to 1.9
- w_gate_b: bfloat16 [2048, 1024], P(('sp', 'fs'), 'tp'), may hold values from -0.125 to 0.125
- w_gate_c: bfloat16 [2048, 1024], P(('sp', 'fs'), 'tp'), may hold values from -0.125 to 0.125
- w_conv_in: bfloat16 [2048, 1024], P(('sp', 'fs'), 'tp'), may hold values from -0.125 to 0.125
- conv_taps: float32 [3, 1024], P(None, 'tp'), may hold values from -3 to 3
- w_out_attn: bfloat16 [1024, 2048], P('tp', ('sp', 'fs')), may hold values from -0.125 to 0.125
- w_out_conv: bfloat16 [1024, 2048], P('tp', ('sp', 'fs')), may hold values from -0.125 to 0.125
Outputs:
- mixed: bfloat16 [8, 512, 2048], P(('grp', 'fs'), ('sp', 'tp')), parts along dimension 0
The draws below stay inside these ranges and needn't reach their ends.
There are 2 independent parts, one for each index of `grp`. The reference program is written for one: setup_inputs(seed, part) draws one part's arguments, and reference() takes and returns one part's arrays. A program takes and returns all parts, laid end to end along the dimension named above; an argument that names none is the same for every part. Nothing has to cross between parts.
All inputs are finite; a program needn't handle non-finite values.
Results may differ from the reference program's by a relative error of at most 0.04.
Values may be sent and summed in bfloat16 or wider, within the bound.
No kernel may reach another device: no remote copies, remote signals or barrier semaphores. Data moves between devices by JAX's collectives and lax.ppermute only.
A program may use at most 128 MiB of HBM per device.

```python
import math
import jax
import jax.numpy as jnp
from jax import lax

D = 2048
HEADS = 8
DK = 64
DV = 128
CW = 1024
KW = 3
SEQ_LEN = 512
SEQS = 4


def draw_tokens(key, part):
    first, second, third = jax.random.split(jax.random.fold_in(key, 11), 3)
    shape = (SEQS, SEQ_LEN, D)
    base = jnp.clip(jax.random.normal(first, shape, jnp.float32), -4.0, 4.0)
    row_scale = jnp.exp(jax.random.uniform(second, (SEQS, SEQ_LEN, 1), jnp.float32, math.log(0.3), math.log(3.0)))
    col_scale = jnp.exp(jax.random.uniform(third, (1, 1, D), jnp.float32, math.log(0.5), math.log(2.0)))
    return (base * row_scale * col_scale).astype(jnp.bfloat16)


def draw_query_gain(key, part):
    first = jax.random.fold_in(jax.random.fold_in(key, 23), 0)
    base = 1.7 * jnp.exp(jax.random.uniform(first, (HEADS, 2, DK), jnp.float32, -0.25, 0.25))
    return base.reshape(HEADS * 2 * DK).astype(jnp.float32)


def block_scale(rng, dims, shards, smallest, high):
    loudness, own = 1.0, jax.random.fold_in(rng, 6)
    for dim, shards_of in shards:
        steps = jnp.exp(jax.random.uniform(jax.random.fold_in(own, dim), (shards_of,), jnp.float32, smallest / len(shards), high / len(shards)))
        loudness = loudness * jnp.repeat(steps, dims[dim] // shards_of).reshape([-1 if axis == dim else 1 for axis in range(len(dims))])
    return loudness


def normal_values(key, shape, spread, bound, pieces=(), held_as=jnp.bfloat16):
    array = jax.random.normal(key, shape, jnp.float32) * spread
    if len(pieces) > 0:
        array = block_scale(key, shape, pieces, -0.22, 0.18) * array
    return jnp.clip(array, min=-bound, max=bound).astype(held_as)


def setup_inputs(seed: int = 0, part: int = 0) -> dict:
    keys = jax.random.split(jax.random.key(seed), 16)
    part_splits = jax.random.split(jax.random.fold_in(keys[15], part), 16)
    tokens = draw_tokens(jax.random.fold_in(jax.random.fold_in(keys[15], part), 71), part)
    norm_gain = jnp.clip(1.0 + 0.18 * jax.random.normal(keys[1], (D,), jnp.float32), 0.1, 1.9)
    w_query = normal_values(keys[2], (D, HEADS * 2 * DK), D ** -0.5, 0.125, ((0, 8), (1, 2)))
    w_key = normal_values(keys[3], (D, HEADS * 2 * DK), D ** -0.5, 0.125, ((0, 8), (1, 2)))
    w_value = normal_values(keys[4], (D, HEADS * DV), D ** -0.5, 0.125, ((0, 8), (1, 2)))
    query_gain = draw_query_gain(jax.random.fold_in(keys[15], 71), part)
    key_gain = jnp.clip(1.0 + 0.18 * jax.random.normal(keys[6], (HEADS * 2 * DK,), jnp.float32), 0.1, 1.9)
    mix_lambda = jnp.clip(0.3 + 0.5 * jax.random.uniform(keys[7], (HEADS,), jnp.float32) ** block_scale(keys[7], (HEADS,), ((0, 2),), -0.2, 0.2), 0.3, 0.8)
    head_gain = jnp.clip(1.0 + 0.18 * jax.random.normal(keys[8], (DV,), jnp.float32), 0.1, 1.9)
    w_gate_b = normal_values(keys[9], (D, CW), D ** -0.5, 0.125, ((0, 8), (1, 2)))
    w_gate_c = normal_values(keys[10], (D, CW), D ** -0.5, 0.125, ((0, 8), (1, 2)))
    w_conv_in = normal_values(keys[11], (D, CW), D ** -0.5, 0.125, ((0, 8), (1, 2)))
    conv_taps = normal_values(keys[12], (KW, CW), 0.577, 3.0, ((1, 2),), jnp.float32)
    w_out_attn = normal_values(keys[13], (HEADS * DV, D), (HEADS * DV + CW) ** -0.5, 0.125, ((0, 2), (1, 8)))
    w_out_conv = normal_values(keys[14], (CW, D), (HEADS * DV + CW) ** -0.5, 0.125, ((0, 2), (1, 8)))
    return dict(tokens=tokens, norm_gain=norm_gain, w_query=w_query, w_key=w_key, w_value=w_value, query_gain=query_gain, key_gain=key_gain, mix_lambda=mix_lambda, head_gain=head_gain, w_gate_b=w_gate_b, w_gate_c=w_gate_c, w_conv_in=w_conv_in, conv_taps=conv_taps, w_out_attn=w_out_attn, w_out_conv=w_out_conv)


EPS = 1e-06
NEG = -1e+30
OUT_SCALE = 0.8

def rms_scale(values, gain):
    wide = values.astype(jnp.float32)
    return wide * lax.rsqrt(lax.optimization_barrier(jnp.mean(wide * wide, axis=-1, keepdims=True)) + EPS) * gain.astype(jnp.float32)

def reference(tokens, norm_gain, w_query, w_key, w_value, query_gain, key_gain, mix_lambda, head_gain, w_gate_b, w_gate_c, w_conv_in, conv_taps, w_out_attn, w_out_conv):
    length = SEQ_LEN
    block = math.gcd(length, 512)

    def one(seq):
        normed = rms_scale(seq, norm_gain).astype(jnp.bfloat16)

        def project(weight):
            return jnp.dot(normed, weight, preferred_element_type=jnp.float32).astype(jnp.bfloat16)
        query = rms_scale(project(w_query).reshape(length, HEADS, 2, DK), query_gain.reshape(HEADS, 2, DK)).astype(jnp.bfloat16)
        key = rms_scale(project(w_key).reshape(length, HEADS, 2, DK), key_gain.reshape(HEADS, 2, DK)).astype(jnp.bfloat16)
        value = project(w_value).reshape(length, HEADS, DV)
        key_wide = key.astype(jnp.float32)
        value_wide = value.astype(jnp.float32)
        key_pos = jnp.arange(length, dtype=jnp.int32)

        def attend(start):
            q_block = lax.dynamic_slice_in_dim(query, start, block, 0).astype(jnp.float32)
            q_pos = start + jnp.arange(block, dtype=jnp.int32)
            score = jnp.einsum('qhmd,khmd->hmqk', q_block, key_wide) * DK ** (-0.5)
            allowed = key_pos[None, :] <= q_pos[:, None]
            score = jnp.where(allowed, score, NEG)
            top = lax.optimization_barrier(jnp.max(score, axis=-1, keepdims=True))
            weights = jnp.exp(score - top)
            total = lax.optimization_barrier(jnp.sum(weights, axis=-1))
            rounded = lax.optimization_barrier(weights.astype(jnp.bfloat16)).astype(jnp.float32)
            summed = jnp.einsum('hmqk,khd->hmqd', rounded, value_wide)
            head_map = summed / total[..., None]
            differ = head_map[:, 0] - mix_lambda.astype(jnp.float32)[:, None, None] * head_map[:, 1]
            normal = rms_scale(differ, head_gain) * OUT_SCALE
            return normal.transpose(1, 0, 2).reshape(block, HEADS * DV).astype(jnp.bfloat16)
        starts = jnp.arange(length // block, dtype=jnp.int32) * block
        attn = lax.map(attend, starts).reshape(length, HEADS * DV)
        gate_b = project(w_gate_b)
        gate_c = project(w_gate_c)
        conv_in = project(w_conv_in)
        shaped = (gate_c.astype(jnp.float32) * conv_in.astype(jnp.float32)).astype(jnp.bfloat16)
        padded = jnp.concatenate([jnp.zeros((KW - 1, CW), jnp.bfloat16), shaped], axis=0).astype(jnp.float32)
        conv = jnp.zeros((length, CW), jnp.float32)
        for tap in range(KW):
            conv = conv + conv_taps[tap].astype(jnp.float32) * padded[tap:tap + length]
        conv_out = (gate_b.astype(jnp.float32) * conv).astype(jnp.bfloat16)
        total_out = jnp.dot(attn, w_out_attn, preferred_element_type=jnp.float32) + jnp.dot(conv_out, w_out_conv, preferred_element_type=jnp.float32)
        return total_out.astype(jnp.bfloat16)
    return lax.map(one, tokens)
```

```python
import math

import jax
import jax.numpy as jnp
from jax import lax
from jax.experimental import pallas as pl
from jax.experimental.pallas import tpu as pltpu
from jax.sharding import PartitionSpec as P

DK = 64
DV = 128
KW = 3


EPS = 1e-06
NEG = -1e30
OUT_SCALE = 0.8


def from_behind(block, axis, distance):
    devices = range(lax.axis_size(axis))
    route = [(i - distance, i) for i in devices if i - distance in devices]
    return lax.ppermute(block, axis, route)


def rms_scale(values, gain):
    wide = values.astype(jnp.float32)
    return wide * lax.rsqrt(jnp.mean(wide * wide, axis=-1, keepdims=True) + EPS) * gain


def attend_heads(normed, wq_full, wk_full, wv_full, query_gain, key_gain, mix_lambda, head_gain):
    rows = normed.shape[0]
    heads_here = mix_lambda.shape[0]
    query = rms_scale(
        jnp.dot(normed, wq_full, preferred_element_type=jnp.float32)
        .astype(jnp.bfloat16)
        .reshape(rows, heads_here, 2, DK),
        query_gain.reshape(heads_here, 2, DK),
    ).astype(jnp.bfloat16)
    key = rms_scale(
        jnp.dot(normed, wk_full, preferred_element_type=jnp.float32)
        .astype(jnp.bfloat16)
        .reshape(rows, heads_here, 2, DK),
        key_gain.reshape(heads_here, 2, DK),
    ).astype(jnp.bfloat16)
    value = jnp.dot(normed, wv_full, preferred_element_type=jnp.float32).astype(jnp.bfloat16)
    q_pos = lax.axis_index("sp") * rows + jnp.arange(rows, dtype=jnp.int32)
    init = (
        jnp.full((heads_here, 2, rows), NEG, jnp.float32),
        jnp.zeros((heads_here, 2, rows), jnp.float32),
        jnp.zeros((heads_here, 2, rows, DV), jnp.float32),
    )
    key_piece = lax.all_gather(key.reshape(rows, heads_here * 2 * DK), "sp", axis=0, tiled=True)
    value_piece = lax.all_gather(value, "sp", axis=0, tiled=True)
    count = key_piece.shape[0]
    width = math.gcd(count, 1024)
    blocks = count // width
    key_blocks = key_piece.reshape(blocks, width, heads_here, 2, DK)
    value_blocks = value_piece.reshape(blocks, width, heads_here, DV)
    begins = jnp.arange(blocks, dtype=jnp.int32) * width

    def step(state, inputs):
        running, total, summed = state
        key_block, value_block, begin = inputs
        k_pos = begin + jnp.arange(width, dtype=jnp.int32)
        score = jnp.einsum(
            "qhmd,khmd->hmqk", query, key_block, preferred_element_type=jnp.float32
        ) * DK ** (-0.5)
        allowed = k_pos[None, :] <= q_pos[:, None]
        score = jnp.where(allowed, score, NEG)
        newest = jnp.maximum(running, jnp.max(score, axis=-1))
        factor = jnp.exp(running - newest)
        weights = jnp.where(allowed, jnp.exp(score - newest[..., None]), 0.0)
        total = total * factor + jnp.sum(weights, axis=-1)
        summed = summed * factor[..., None] + jnp.einsum(
            "hmqk,khd->hmqd",
            weights.astype(jnp.bfloat16),
            value_block,
            preferred_element_type=jnp.float32,
        )
        return ((newest, total, summed), None)

    result, unused = lax.scan(step, init, (key_blocks, value_blocks, begins))
    running, total, summed = result
    head_map = summed / total[..., None]
    differ = head_map[:, 0] - mix_lambda[:, None, None] * head_map[:, 1]
    normal = rms_scale(differ, head_gain) * OUT_SCALE
    return normal.transpose(1, 0, 2).reshape(rows, heads_here * DV).astype(jnp.bfloat16)


def gated_conv(normed, wb_full, wc_full, wi_full, conv_taps):
    rows = normed.shape[0]
    gate_b = jnp.dot(normed, wb_full, preferred_element_type=jnp.float32).astype(jnp.bfloat16)
    gate_c = jnp.dot(normed, wc_full, preferred_element_type=jnp.float32).astype(jnp.bfloat16)
    conv_in = jnp.dot(normed, wi_full, preferred_element_type=jnp.float32).astype(jnp.bfloat16)
    shaped = (gate_c.astype(jnp.float32) * conv_in.astype(jnp.float32)).astype(jnp.bfloat16)
    edge = from_behind(shaped[rows - (KW - 1) :], "sp", 1)
    padded = jnp.concatenate([edge, shaped], axis=0).astype(jnp.float32)
    conv = conv_taps[0][None, :] * padded[0:rows]
    for tap in range(1, KW):
        conv = conv + conv_taps[tap][None, :] * padded[tap : tap + rows]
    return (gate_b.astype(jnp.float32) * conv).astype(jnp.bfloat16)


def normalize_rows(own_rows, norm_gain):
    return rms_scale(lax.all_gather(own_rows, "tp", axis=0, tiled=True), norm_gain).astype(
        jnp.bfloat16
    )


def on_device(
    tokens,
    norm_gain,
    w_query,
    w_key,
    w_value,
    query_gain,
    key_gain,
    mix_lambda,
    head_gain,
    w_gate_b,
    w_gate_c,
    w_conv_in,
    conv_taps,
    w_out_attn,
    w_out_conv,
):
    seq_count = tokens.shape[0]
    gathered = (
        lax.all_gather(w_query, ("sp", "fs"), axis=0, tiled=True),
        lax.all_gather(w_key, ("sp", "fs"), axis=0, tiled=True),
        lax.all_gather(w_value, ("sp", "fs"), axis=0, tiled=True),
        lax.all_gather(w_gate_b, ("sp", "fs"), axis=0, tiled=True),
        lax.all_gather(w_gate_c, ("sp", "fs"), axis=0, tiled=True),
        lax.all_gather(w_conv_in, ("sp", "fs"), axis=0, tiled=True),
        lax.all_gather(w_out_attn, ("sp", "fs"), axis=1, tiled=True),
        lax.all_gather(w_out_conv, ("sp", "fs"), axis=1, tiled=True),
    )
    normed_list = [normalize_rows(tokens[index], norm_gain) for index in range(seq_count)]
    attn_list = [
        attend_heads(
            normed,
            gathered[0],
            gathered[1],
            gathered[2],
            query_gain,
            key_gain,
            mix_lambda,
            head_gain,
        )
        for normed in normed_list
    ]
    conv_list = [
        gated_conv(normed, gathered[3], gathered[4], gathered[5], conv_taps)
        for normed in normed_list
    ]
    out_attn = gathered[6]
    out_conv = gathered[7]
    results = []
    for index in range(seq_count):
        attn = attn_list[index]
        conv_out = conv_list[index]
        results.append(
            lax.psum_scatter(
                (
                    jnp.dot(attn, out_attn, preferred_element_type=jnp.float32)
                    + jnp.dot(conv_out, out_conv, preferred_element_type=jnp.float32)
                ).astype(jnp.bfloat16),
                "tp",
                scatter_dimension=0,
                tiled=True,
            )
        )
    return jnp.stack(results, axis=0)


BF16, F32 = jnp.bfloat16, jnp.float32
ANY = pl.BlockSpec(memory_space=pl.ANY)
VMEM = pl.BlockSpec(memory_space=pltpu.VMEM)
SMEM = pl.BlockSpec(memory_space=pltpu.SMEM)
SWAP = [(0, 1), (1, 0)]


def source_of(shift, levels):
    return lax.rem(lax.axis_index("sp") + (levels - shift), levels)


def mixer_kernel(
    levels, steps, seqs, half, *refs
):
    n_x = 2 * levels
    n_w = 8
    x_refs = refs[:n_x]
    w_refs = refs[n_x : n_x + n_w]
    norm_gain, qg, kg, lam, hg, taps = refs[n_x + n_w : n_x + n_w + 6]
    z_ref = refs[n_x + n_w + 6]
    x_scr, w_scr, n_scr, p_scr, x_sem, w_sem = refs[n_x + n_w + 7 :]
    s = lax.axis_index("sp")
    g = lax.axis_index("grp")
    f = lax.axis_index("fs")
    t = lax.axis_index("tp")
    rows = 2 * half
    length = levels * rows
    n_f = steps
    depth = w_refs[0].shape[2]
    width = w_refs[0].shape[3]

    x_copies = []
    for k in range(levels):
        src = source_of(k, levels)
        group = []
        for o in range(2):
            side = t if o == 0 else 1 - t
            for b in range(seqs):
                at = pl.multiple_of(src * (seqs * rows) + b * rows + side * half, half)
                c = pltpu.make_async_copy(
                    x_refs[o * levels + k].at[b],
                    x_scr.at[pl.ds(at, half), :],
                    x_sem.at[k, o, b],
                )
                c.start()
                group.append(c)
        x_copies.append(group)
    w_copies = []
    for i in range(n_w):
        ty = g if i < 4 else 1 - g
        fs = f if i % 4 < 2 else 1 - f
        h = i % 2
        for j in range(2):
            src = source_of(2 * h + j, levels)
            at = pl.multiple_of((src * n_f + fs) * depth, depth)
            for w in range(3):
                c = pltpu.make_async_copy(
                    w_refs[i].at[j, w],
                    w_scr.at[ty, pl.ds(at, depth), pl.ds(w * width, width)],
                    w_sem.at[i, j, w],
                )
                c.start()
                w_copies.append(c)
    gain = norm_gain[...]
    step = 16
    for k in range(levels):
        for c in x_copies[k]:
            c.wait()
        base = source_of(k, levels) * (seqs * rows)

        @pl.loop(0, seqs * rows // step, unroll=2)
        def _(n):
            at = pl.multiple_of(base + n * step, step)
            wide = x_scr[pl.ds(at, step), :].astype(F32)
            scale = lax.rsqrt(jnp.mean(wide * wide, axis=-1, keepdims=True) + EPS)
            n_scr[pl.ds(at, step), :] = (wide * scale * gain).astype(BF16)

    for c in w_copies:
        c.wait()
    lane = lax.broadcasted_iota(jnp.int32, (1, 2 * DK), 1)
    first = lane < DK

    def pair_norm(raw, own_gain):
        wide = raw.astype(BF16).astype(F32)
        sq = wide * wide
        m0 = jnp.sum(jnp.where(first, sq, 0.0), axis=-1, keepdims=True) * (1.0 / DK)
        m1 = jnp.sum(jnp.where(first, 0.0, sq), axis=-1, keepdims=True) * (1.0 / DK)
        return wide * jnp.where(first, lax.rsqrt(m0 + EPS), lax.rsqrt(m1 + EPS)) * own_gain

    q_gain = qg[pl.ds(s, 1), :]
    k_gain = kg[pl.ds(s, 1), :]
    for level in range(levels):
        at = level * seqs * rows
        normed = n_scr[at : at + seqs * rows, :]
        for ty in range(2):
            got = jnp.dot(normed, w_scr[ty], preferred_element_type=F32)
            parts = [got[:, w * width : (w + 1) * width] for w in range(3)]
            if ty == 0:
                parts[0] = pair_norm(parts[0], q_gain) * DK ** (-0.5)
                parts[1] = pair_norm(parts[1], k_gain)
            for w in range(3):
                done = parts[w].astype(BF16)
                for b in range(seqs):
                    p_scr[3 * ty + w, b, level * rows : (level + 1) * rows, :] = done[
                        b * rows : (b + 1) * rows
                    ]
    lam_own = lam[s]
    head_gain = hg[...]
    row = lax.broadcasted_iota(jnp.int32, (rows, rows), 0)
    col = lax.broadcasted_iota(jnp.int32, (rows, rows), 1)
    seen = col <= row
    seen = jnp.concatenate([seen, seen], axis=0)
    for b in range(seqs):
        shaped = (p_scr[4, b].astype(F32) * p_scr[5, b].astype(F32)).astype(BF16).astype(F32)
        where = lax.broadcasted_iota(jnp.int32, (length, 1), 0)
        conv = taps[KW - 1, pl.ds(s, 1), :] * shaped
        for back in range(1, KW):
            moved = jnp.where(where >= back, pltpu.roll(shaped, back, 0), 0.0)
            conv = conv + taps[KW - 1 - back, pl.ds(s, 1), :] * moved
        conv_out = (p_scr[3, b].astype(F32) * conv).astype(BF16)
        for i in range(levels):
            to = lax.rem(i - s + levels, levels)
            z_ref[to, b, :, width:] = conv_out[i * rows : (i + 1) * rows]
            q = p_scr[0, b, i * rows : (i + 1) * rows, :]
            zero = jnp.zeros_like(q)
            q2 = jnp.concatenate([jnp.where(first, q, zero), jnp.where(first, zero, q)], axis=0)
            upto = (i + 1) * rows
            score = lax.dot_general(
                q2,
                p_scr[1, b, :upto, :],
                (((1,), (1,)), ((), ())),
                preferred_element_type=F32,
            )
            edge = jnp.where(seen, score[:, i * rows :], NEG)
            if i > 0:
                score = jnp.concatenate([score[:, : i * rows], edge], axis=1)
            else:
                score = edge
            top = jnp.max(score, axis=-1, keepdims=True)
            weights = jnp.exp(score - top)
            total = jnp.sum(weights, axis=-1, keepdims=True)
            summed = jnp.dot(
                weights.astype(BF16), p_scr[2, b, :upto, :], preferred_element_type=F32
            )
            maps = summed / total
            differ = maps[:rows] - lam_own * maps[rows:]
            scale = lax.rsqrt(jnp.mean(differ * differ, axis=-1, keepdims=True) + EPS)
            z_ref[to, b, :, :width] = (differ * scale * head_gain * OUT_SCALE).astype(BF16)


def output_kernel(levels, steps, seqs, half, *refs):
    z_refs = refs[:levels]
    w_refs = refs[levels : levels + 8]
    keep_ref, send_ref = refs[levels + 8 : levels + 10]
    z_scr, w_scr, w_sem = refs[levels + 10 :]
    g = lax.axis_index("grp")
    f = lax.axis_index("fs")
    t = lax.axis_index("tp")
    rows = 2 * half
    width = z_refs[0].shape[2] // 2
    columns = w_refs[0].shape[2]
    copies = []
    for i in range(8):
        ty = g if i < 4 else 1 - g
        pair = []
        for j in range(2):
            c = pltpu.make_async_copy(w_refs[i].at[j], w_scr.at[ty, i % 4, j], w_sem.at[i, j])
            c.start()
            pair.append(c)
        copies.append(pair)
    for k in range(levels):
        at = pl.multiple_of(source_of(k, levels) * width, width)
        for b in range(seqs):
            for ty in range(2):
                z_scr[ty, b * rows : (b + 1) * rows, pl.ds(at, width)] = z_refs[k][
                    b, :, ty * width : (ty + 1) * width
                ]
    for q in range(4):
        fs = f if q < 2 else 1 - f
        for j in range(2):
            copies[q][j].wait()
            copies[q + 4][j].wait()
            got = jnp.dot(z_scr[0], w_scr[0, q, j], preferred_element_type=F32) + jnp.dot(
                z_scr[1], w_scr[1, q, j], preferred_element_type=F32
            )
            src = source_of(2 * (q % 2) + j, levels)
            at = pl.multiple_of((src * steps + fs) * columns, columns)
            for b in range(seqs):
                low = got[b * rows : b * rows + half]
                high = got[b * rows + half : (b + 1) * rows]
                keep_ref[b, :, pl.ds(at, columns)] = jnp.where(t == 0, low, high)
                send_ref[b, :, pl.ds(at, columns)] = jnp.where(t == 0, high, low).astype(BF16)


def both_ways(halves):
    first, second = halves
    first_x = lax.ppermute(first, "fs", SWAP)
    second_y = lax.ppermute(second, "grp", SWAP)
    first_y = lax.ppermute(first, "grp", SWAP)
    second_x = lax.ppermute(second, "fs", SWAP)
    first_xy = lax.ppermute(first_x, "grp", SWAP)
    second_xy = lax.ppermute(second_y, "fs", SWAP)
    return [first, second, first_x, second_x, first_y, second_y, first_xy, second_xy]


def relayed_device(
    tokens,
    norm_gain,
    w_query,
    w_key,
    w_value,
    query_gain,
    key_gain,
    mix_lambda,
    head_gain,
    w_gate_b,
    w_gate_c,
    w_conv_in,
    conv_taps,
    w_out_attn,
    w_out_conv,
):
    levels = lax.axis_size("sp")
    steps = lax.axis_size("fs")
    s = lax.axis_index("sp")
    g = lax.axis_index("grp")
    seqs, half, model = tokens.shape
    depth, wide = w_query.shape
    width = wide // levels
    up = [(i, i + 1) for i in range(levels - 1)]
    down = [(i + 1, i) for i in range(levels - 1)]

    def shifted(block, k):
        return lax.ppermute(block, "sp", [(i, (i + k) % levels) for i in range(levels)])

    from_below = [tokens]
    from_above = [tokens]
    from_below.append(lax.ppermute(from_below[-1], "sp", up))
    from_above.append(lax.ppermute(from_above[-1], "sp", down))

    mine = jnp.where(
        g == 0, jnp.stack([w_query, w_key, w_value]), jnp.stack([w_gate_b, w_gate_c, w_conv_in])
    )
    pieces = []
    for k in range(levels):
        at = lax.rem(s + k, levels) * width
        piece = lax.dynamic_slice(mine, (0, 0, at), (3, depth, width))
        pieces.append(shifted(piece, k) if k else piece)
    w_parts = both_ways([jnp.stack(pieces[:2]), jnp.stack(pieces[2:])])

    own_out = jnp.where(g == 0, w_out_attn, w_out_conv)
    outs = [own_out] + [shifted(own_out, k) for k in range(1, levels)]
    o_parts = both_ways([jnp.stack(outs[:2]), jnp.stack(outs[2:])])

    for k in range(2, levels):
        from_below.append(lax.ppermute(from_below[-1], "sp", up))
        from_above.append(lax.ppermute(from_above[-1], "sp", down))
    blocks = [tokens] + [
        jnp.where(s >= k, from_below[k], from_above[levels - k]) for k in range(1, levels)
    ]
    others = [lax.ppermute(block, "tp", SWAP) for block in blocks]

    z = pl.pallas_call(
        lambda *refs: mixer_kernel(levels, steps, seqs, half, *refs),
        out_shape=jax.ShapeDtypeStruct((levels, seqs, 2 * half, 2 * width), BF16),
        in_specs=[ANY] * (2 * levels + 8) + [VMEM, VMEM, VMEM, SMEM, VMEM, VMEM],
        out_specs=VMEM,
        scratch_shapes=[
            pltpu.VMEM((levels * seqs * 2 * half, model), BF16),
            pltpu.VMEM((2, model, 3 * width), BF16),
            pltpu.VMEM((levels * seqs * 2 * half, model), BF16),
            pltpu.VMEM((6, seqs, levels * 2 * half, width), BF16),
            pltpu.SemaphoreType.DMA((levels, 2, seqs)),
            pltpu.SemaphoreType.DMA((8, 2, 3)),
        ],
        compiler_params=pltpu.CompilerParams(vmem_limit_bytes=48 * 1024 * 1024),
        cost_estimate=pl.CostEstimate(
            flops=8_000_000_000, bytes_accessed=8_000_000, transcendentals=1_000_000
        ),
        name="mixer",
    )(
        *blocks,
        *others,
        *w_parts,
        norm_gain.reshape(1, model),
        query_gain.reshape(levels, 2 * DK),
        key_gain.reshape(levels, 2 * DK),
        mix_lambda,
        head_gain.reshape(1, DV),
        conv_taps.reshape(KW, levels, width),
    )
    arrived = [z[0]] + [shifted(z[k], k) for k in range(1, levels)]
    keep, send = pl.pallas_call(
        lambda *refs: output_kernel(levels, steps, seqs, half, *refs),
        out_shape=(
            jax.ShapeDtypeStruct((seqs, half, model), F32),
            jax.ShapeDtypeStruct((seqs, half, model), BF16),
        ),
        in_specs=[VMEM] * levels + [ANY] * 8,
        out_specs=(VMEM, VMEM),
        scratch_shapes=[
            pltpu.VMEM((2, seqs * 2 * half, wide), BF16),
            pltpu.VMEM((2, 4, 2, wide, w_out_attn.shape[1]), BF16),
            pltpu.SemaphoreType.DMA((8, 2)),
        ],
        compiler_params=pltpu.CompilerParams(vmem_limit_bytes=32 * 1024 * 1024),
        cost_estimate=pl.CostEstimate(
            flops=2_000_000_000, bytes_accessed=8_000_000, transcendentals=0
        ),
        name="output",
    )(*arrived, *o_parts)
    return (keep + lax.ppermute(send, "tp", SWAP).astype(F32)).astype(BF16)


def solution(mesh):
    placed = (
        P(("grp", "fs"), ("sp", "tp"), None),
        P(),
        P(("sp", "fs"), "tp"),
        P(("sp", "fs"), "tp"),
        P(("sp", "fs"), "tp"),
        P("tp"),
        P("tp"),
        P("tp"),
        P(),
        P(("sp", "fs"), "tp"),
        P(("sp", "fs"), "tp"),
        P(("sp", "fs"), "tp"),
        P(None, "tp"),
        P("tp", ("sp", "fs")),
        P("tp", ("sp", "fs")),
    )
    grid = mesh.shape
    relayed = grid["grp"] == 2 and grid["fs"] == 2 and grid["tp"] == 2 and grid["sp"] == 4

    def layer(*arrays):
        alike = arrays[2].shape == arrays[4].shape == arrays[9].shape
        one_head = arrays[7].shape[0] == grid["sp"] * grid["tp"]
        if relayed and alike and one_head:
            body = relayed_device
        else:
            body = on_device
        return sharded(body)(*arrays)

    sharded = lambda body: jax.shard_map(
        body,
        mesh=mesh,
        in_specs=placed,
        out_specs=P(("grp", "fs"), ("sp", "tp"), None),
        check_vma=False,
    )
    return layer
```
